128 devices in a mesh: sp: 32 (over z, y, core), tp: 4 (over x).
Axes of the slice: x: 4, y: 4, z: 4, core: 2. Of those that a mesh axis runs over, the one named last changes fastest.
Arguments:
- residual_in: bfloat16 [65536, 2048], P(('sp', 'tp')), may hold values from -6 to 6
- conv_input: bfloat16 [65536, 1024], P('sp', 'tp'), may hold values from -6 to 6
- input_gate: bfloat16 [65536, 1024], P('sp', 'tp'), may hold values from -6 to 6
- output_gate: bfloat16 [65536, 1024], P('sp', 'tp'), may hold values from -6 to 6
- conv_taps: bfloat16 [3, 1024], P(None, 'tp'), may hold values from -3.5 to 3.5
- doc_ids: int32 [65536], P('sp'), may hold values from 0 to 15, never falling along the last dimension, each value on 1 to 8192 neighbouring positions
- proj_weight: bfloat16 [1024, 2048], replicated, may hold values from -0.1875 to 0.1875
- norm_gain: float32 [2048], replicated, may hold values from 0.1 to 1.9
- expert_ids: int32 [65536, 2], P(('sp', 'tp')), may hold values from 0 to 31, all different within a row; in each aligned block of 512 rows (0 to 511, 512 to 1023, ...) at most 64 rows name the same one
- expert_weight: float32 [65536, 2], P(('sp', 'tp')), may hold values from 0.05 to 1
- w_gate: bfloat16 [32, 2048, 512], P('sp'), may hold values from -0.125 to 0.125
- w_up: bfloat16 [32, 2048, 512], P('sp'), may hold values from -0.125 to 0.125
- w_down: bfloat16 [32, 512, 2048], P('sp'), may hold values from -0.25 to 0.25
Outputs:
- layer_out: bfloat16 [65536, 2048], P(('sp', 'tp'))
The draws below stay inside these ranges and needn't reach their ends.
Inputs may be any that keep to these rules, and one draw needn't show every extreme that they name: `doc_ids`: numbers never fall along the sequence; one document spans at most 8192 positions. `expert_ids`: a token's two experts differ; in each aligned block of rows that one device holds, no expert is named more than 64 times, a bound that some block reaches.
All inputs are finite; a program needn't handle non-finite values.
Results may differ from the reference program's by a relative error of at most 0.0047.
Values may be sent and summed in bfloat16 or wider, within the bound.
No kernel may reach another device: no remote copies, remote signals or barrier semaphores. Data moves between devices by JAX's collectives and lax.ppermute only.
A program may use at most 128 MiB of HBM per device.

```python
import math
import jax
import jax.numpy as jnp
import numpy as np
from jax import lax

D = 2048
CONV = 1024
FFE = 512
EXPERTS = 32
KW = 3
CAP = 64
TOK_DEV = 2048
TOKENS = 65536
SEG_COUNT = 16
DOC_MOST = 8192
N_SP = 32
N_TP = 4


def block_scale(rng, dims, cuts, smallest, high):
    def one(dim, parts):
        heights = jax.random.uniform(jax.random.fold_in(jax.random.fold_in(rng, 6), dim), (parts,), jnp.float32, smallest / len(cuts), high / len(cuts))
        return jnp.repeat(jnp.exp(heights), dims[dim] // parts).reshape((-1,) + (1,) * (len(dims) - dim - 1))

    loudness = one(*cuts[0])
    for cut in cuts[1:]:
        loudness = loudness * one(*cut)
    return loudness


def profile(amount, total, limit, skew):
    loads = [(1 << 20) // math.isqrt(grade ** skew) + 1 for grade in range(2, amount + 1)]
    surplus, holding = total - limit - (amount - 1), [1] * (amount - 1)
    while surplus > 0:
        free = [i for i in range(amount - 1) if holding[i] < limit]
        mass, budget = sum([loads[i] for i in free]), surplus
        for i in free:
            more = min(limit - holding[i], max(1, budget * loads[i] // mass), surplus)
            holding[i] = holding[i] + more
            surplus = surplus - more
    return np.array([limit] + holding)


def ragged_sizes(stream_key, number_of, total, reach, skew):
    if number_of == 2:
        one = jax.random.randint(stream_key, (), max(1, total - reach), min(reach, total - 1) + 1)
        return jnp.stack([one, total - one])
    sizes = jnp.asarray(profile(number_of, total, reach, skew), jnp.int32)
    couples = (number_of - 1) // 2
    giver, receiver = sizes[1:1 + 2 * couples:2], sizes[2:2 + 2 * couples:2]
    room = jnp.minimum(giver - 1, reach - receiver)
    moved = jax.random.randint(jax.random.fold_in(stream_key, 1), (couples,), 0, 1 << 20) % (room + 1)
    sizes = sizes.at[1:1 + 2 * couples:2].set(giver - moved).at[2:2 + 2 * couples:2].set(receiver + moved)
    return sizes[jax.random.permutation(jax.random.fold_in(stream_key, 2), number_of)]


def assign_block(rng, own, number, rows, number_of, top, bound, lean):
    ranking = jax.random.permutation(rng, number_of)
    packed, common = shares(number_of, rows * top, bound, lean, True), shares(number_of, rows * top, bound, lean, False)
    places = jnp.arange(number_of)

    def named(sizes, turn):
        used = int((sizes > 0).sum())
        fixed = max(1, used // 4)
        passed = fixed + (places - fixed + turn * (used - fixed)) % max(1, number_of - fixed)
        return jnp.zeros((number_of,), jnp.int32).at[ranking[jnp.where(places < fixed, places, passed)]].set(jnp.asarray(sizes, jnp.int32))

    sizes = jnp.where(number % 4 == 0, named(packed, number // 4), named(common, number - number // 4 - 1))
    mixed = jax.random.permutation(jax.random.fold_in(own, 3), number_of)
    donor, taker = mixed[0:number_of // 2 * 2:2], mixed[1:number_of // 2 * 2:2]
    slack = jnp.minimum(sizes[donor] - 1, bound - sizes[taker]) // 2
    slack = jnp.where((donor == ranking[0]) | (taker == ranking[0]) | (sizes[taker] == 0), 0, jnp.maximum(slack, 0))
    passed = jax.random.randint(jax.random.fold_in(own, 4), (number_of // 2,), 0, 1 << 20) % (slack + 1)
    sizes = sizes.at[donor].add(-passed).at[taker].add(passed)
    labels = jnp.searchsorted(jnp.cumsum(sizes), jnp.arange(rows * top), side="right").astype(jnp.int32)
    listing = labels.reshape(top, rows).T
    listing = listing[jax.random.permutation(jax.random.fold_in(own, 1), rows)]
    turn = jax.random.randint(jax.random.fold_in(own, 2), (rows, 1), 0, top)
    return jnp.take_along_axis(listing, (jnp.arange(top)[None, :] + turn) % top, axis=1)


def shares(amount, total, most, skew, full):
    weights = [(1 << 20) // math.isqrt(standing ** skew) + 1 for standing in range(1, amount + 1)]
    largest = most if full else min(most, max(-(-total // amount), total * weights[0] // sum(weights)))
    least = 1 if total - largest >= amount - 1 else 0
    counts, spare = [largest] + [least] * (amount - 1), total - largest - least * (amount - 1)
    while spare > 0:
        movable = [i for i in range(1, amount) if counts[i] < largest] or [i for i in range(1, amount) if counts[i] < most]
        mass, budget = sum([weights[i] for i in movable]), spare
        for i in movable:
            addition = min(most - counts[i], max(1, budget * weights[i] // mass), spare)
            counts[i] = counts[i] + addition
            spare = spare - addition
    return np.array(counts)


def centred(rng, extent, width, most, split=(), kind=jnp.bfloat16):
    values = width * jax.random.normal(rng, extent, jnp.float32)
    if split:
        values = values * block_scale(rng, extent, split, -0.22, 0.18)
    return jnp.clip(values, -most, most).astype(kind)


def setup_inputs(seed: int = 0) -> dict:
    key_of = jax.random.split(jax.random.key(seed), 14)
    residual_in = centred(key_of[0], (TOKENS, D), 1.0, 6.0, ((0, 128),))
    conv_input = centred(key_of[1], (TOKENS, CONV), 1.0, 6.0, ((0, 32), (1, 4)))
    input_gate = centred(key_of[2], (TOKENS, CONV), 1.0, 6.0, ((0, 32), (1, 4)))
    output_gate = centred(key_of[3], (TOKENS, CONV), 1.0, 6.0, ((0, 32), (1, 4)))
    conv_taps = centred(key_of[4], (KW, CONV), KW ** -0.5, 3.5, ((1, 4),))
    doc_ids = jnp.searchsorted(jnp.cumsum(ragged_sizes(key_of[5], SEG_COUNT, TOKENS, DOC_MOST, 2)), jnp.arange(TOKENS), side="right").astype(jnp.int32)
    proj_weight = centred(key_of[6], (CONV, D), CONV ** -0.5, 0.1875)
    norm_gain = jnp.clip(1.0 + 0.18 * jax.random.normal(key_of[7], (D,), jnp.float32), 0.1, 1.9)
    expert_ids_keys = jax.random.split(jax.random.fold_in(key_of[8], 1), TOKENS // (TOK_DEV // N_TP))
    expert_ids_turns = jax.random.permutation(jax.random.fold_in(key_of[8], 3), TOKENS // (TOK_DEV // N_TP))
    expert_ids = jax.vmap(lambda own, number: assign_block(jax.random.fold_in(key_of[8], 2), own, number, TOK_DEV // N_TP, EXPERTS, 2, CAP, 2))(expert_ids_keys, expert_ids_turns).reshape((TOKENS, 2))
    expert_weight = jnp.clip(jnp.exp(math.log(1.0) - 2.9957323 * jax.random.uniform(key_of[9], (TOKENS, 2), jnp.float32) ** block_scale(key_of[9], (TOKENS, 2), ((0, 128),), -0.2, 0.2)), 0.05, 1.0)
    w_gate = centred(key_of[10], (EXPERTS, D, FFE), D ** -0.5, 0.125, ((0, 32),))
    w_up = centred(key_of[11], (EXPERTS, D, FFE), D ** -0.5, 0.125, ((0, 32),))
    w_down = centred(key_of[12], (EXPERTS, FFE, D), FFE ** -0.5, 0.25, ((0, 32),))
    return dict(residual_in=residual_in, conv_input=conv_input, input_gate=input_gate, output_gate=output_gate, conv_taps=conv_taps, doc_ids=doc_ids, proj_weight=proj_weight, norm_gain=norm_gain, expert_ids=expert_ids, expert_weight=expert_weight, w_gate=w_gate, w_up=w_up, w_down=w_down)


epsilon = 1e-06

def reference(residual_in, conv_input, input_gate, output_gate, conv_taps, doc_ids, proj_weight, norm_gain, expert_ids, expert_weight, w_gate, w_up, w_down):
    product = input_gate.astype(jnp.float32) * conv_input.astype(jnp.float32)
    padded_in = jnp.concatenate([jnp.zeros((KW - 1, CONV), jnp.float32), product], axis=0)
    padded_ids = jnp.concatenate([jnp.full((KW - 1,), -1, jnp.int32), doc_ids.astype(jnp.int32)], axis=0)
    conv_sum = jnp.zeros((TOKENS, CONV), jnp.float32)
    for offset in range(KW):
        same_doc = padded_ids[offset:offset + TOKENS] == doc_ids
        term = conv_taps[offset].astype(jnp.float32)[None, :] * padded_in[offset:offset + TOKENS]
        conv_sum = conv_sum + jnp.where(same_doc[:, None], term, 0.0)
    gated = (output_gate.astype(jnp.float32) * conv_sum).astype(jnp.bfloat16)
    hidden = residual_in.astype(jnp.float32) + jnp.dot(gated, proj_weight, preferred_element_type=jnp.float32)
    scale_rows = lax.rsqrt(lax.optimization_barrier(jnp.mean(hidden * hidden, axis=-1, keepdims=True)) + epsilon)
    normed = (hidden * scale_rows * norm_gain[None, :]).astype(jnp.bfloat16)
    blocks = N_SP * N_TP
    block_rows = TOK_DEV // N_TP
    slots_all = blocks * CAP
    flat_ids = expert_ids.reshape(blocks, 2 * block_rows)
    one_hot = (flat_ids[:, :, None] == jnp.arange(EXPERTS, dtype=jnp.int32)[None, None, :]).astype(jnp.int32)
    before = jnp.cumsum(one_hot, axis=1) - one_hot
    slot_num = lax.optimization_barrier(jnp.sum(before * one_hot, axis=-1))
    slot_index = (jnp.arange(blocks, dtype=jnp.int32)[:, None] * CAP + slot_num).reshape(TOKENS, 2).astype(jnp.int32)

    def per_expert(total, expert):
        chosen = expert_ids == expert
        target = jnp.where(chosen, slot_index, slots_all)
        buffer = jnp.zeros((slots_all, D), jnp.bfloat16)
        buffer = buffer.at[target[:, 0]].set(normed, mode='drop')
        buffer = buffer.at[target[:, 1]].set(normed, mode='drop')
        gate_val = jnp.dot(buffer, w_gate[expert], preferred_element_type=jnp.float32)
        up_val = jnp.dot(buffer, w_up[expert], preferred_element_type=jnp.float32)
        act_rows = (jax.nn.silu(gate_val) * up_val).astype(jnp.bfloat16)
        out_rows = jnp.dot(act_rows, w_down[expert], preferred_element_type=jnp.float32).astype(jnp.bfloat16)
        for route in range(2):
            picked = out_rows[slot_index[:, route]].astype(jnp.float32) * expert_weight[:, route:route + 1]
            total = total + jnp.where(chosen[:, route:route + 1], picked, 0.0)
        return (total, None)
    expert_sum, unused = lax.scan(per_expert, jnp.zeros((TOKENS, D), jnp.float32), jnp.arange(EXPERTS, dtype=jnp.int32))
    return (hidden + expert_sum).astype(jnp.bfloat16)
```

```python
import jax
import jax.numpy as jnp
from jax import lax
from jax.sharding import PartitionSpec as P

EXPERTS = 32
CAP = 64
CHUNKS = 1

epsilon = 1e-06
f32 = jnp.float32
bf16 = jnp.bfloat16


def from_behind(x, axis, by):
    devices = lax.axis_size(axis)
    pairs = [(i, i + by) for i in range(devices) if 0 <= i + by < devices]
    return lax.ppermute(x, axis, pairs)


def exchange(x, axis):
    return lax.all_to_all(x, axis, split_axis=0, concat_axis=0, tiled=True)


def per_device(
    residual_in,
    conv_input,
    input_gate,
    output_gate,
    conv_taps,
    doc_ids,
    proj_weight,
    norm_gain,
    expert_ids,
    expert_weight,
    w_gate,
    w_up,
    w_down,
):
    width = residual_in.shape[1]
    tokens = residual_in.shape[0]
    length, channels = conv_input.shape
    rim = conv_taps.shape[0] - 1

    doc_float = doc_ids.astype(f32)
    tail = input_gate[-rim:].astype(f32) * conv_input[-rim:].astype(f32)
    packed = jnp.concatenate([tail, jnp.broadcast_to(doc_float[-rim:, None], (rim, 128))], axis=1)
    behind = from_behind(packed, "sp", 1)
    product = input_gate.astype(f32) * conv_input.astype(f32)
    padded_in = jnp.concatenate([behind[:, :channels], product], axis=0)
    padded_ids = jnp.concatenate([behind[:, channels], doc_float], axis=0)
    conv_sum = jnp.zeros(product.shape, f32)
    for offset in range(rim + 1):
        same_doc = padded_ids[offset : offset + length] == doc_float
        term = conv_taps[offset].astype(f32)[None, :] * padded_in[offset : offset + length]
        conv_sum = conv_sum + jnp.where(same_doc[:, None], term, 0.0)
    gated = (output_gate.astype(f32) * conv_sum).astype(bf16)
    regrouped = lax.all_to_all(gated, "tp", split_axis=0, concat_axis=1, tiled=True)

    experts = jnp.arange(EXPERTS, dtype=jnp.int32)
    named = expert_ids[:, :, None] == experts[None, None, :]
    chosen = jnp.any(named, axis=1)
    weight = jnp.sum(jnp.where(named, expert_weight[:, :, None], 0.0), axis=1)
    earlier = (jnp.arange(tokens)[:, None] > jnp.arange(tokens)[None, :]).astype(bf16)
    rank = jnp.dot(earlier, chosen.astype(bf16), preferred_element_type=f32)
    code = jnp.where(chosen, rank, -1.0)
    code_t = code.T

    mixed = jnp.dot(regrouped, proj_weight, preferred_element_type=f32)
    hidden = residual_in.astype(f32) + mixed
    scale_rows = lax.rsqrt(jnp.mean(hidden * hidden, axis=-1, keepdims=True) + epsilon)
    normed = (hidden * scale_rows * norm_gain[None, :]).astype(bf16)

    size = CAP // CHUNKS
    rows = EXPERTS * size
    sent = []
    for k in range(CHUNKS):
        ranks = (jnp.arange(size) + k * size).astype(f32)
        pick = (code_t[:, None, :] == ranks[None, :, None]).reshape(rows, tokens).astype(bf16)
        slots = jnp.dot(pick, normed, preferred_element_type=f32).astype(bf16)
        sent.append(exchange(slots.reshape(EXPERTS, size, width), "sp"))
    back = []
    for k in range(CHUNKS):
        slots = sent[k].reshape(rows, width)
        gate_val = jnp.dot(slots, w_gate[0], preferred_element_type=f32)
        up_val = jnp.dot(slots, w_up[0], preferred_element_type=f32)
        act_rows = (jax.nn.silu(gate_val) * up_val).astype(bf16)
        expert_out = jnp.dot(act_rows, w_down[0], preferred_element_type=f32).astype(bf16)
        back.append(exchange(expert_out.reshape(EXPERTS, size, width), "sp"))
    total = hidden
    for k in range(CHUNKS):
        ranks = (jnp.arange(size) + k * size).astype(f32)
        place = jnp.where(code[:, :, None] == ranks[None, None, :], weight[:, :, None], 0.0)
        place = place.reshape(tokens, rows).astype(bf16)
        total = total + jnp.dot(place, back[k].reshape(rows, width), preferred_element_type=f32)
    return total.astype(bf16)


def solution(mesh):
    return jax.shard_map(
        per_device,
        mesh=mesh,
        in_specs=(
            P(("sp", "tp"), None),
            P("sp", "tp"),
            P("sp", "tp"),
            P("sp", "tp"),
            P(None, "tp"),
            P("sp"),
            P(),
            P(),
            P(("sp", "tp"), None),
            P(("sp", "tp"), None),
            P("sp", None, None),
            P("sp", None, None),
            P("sp", None, None),
        ),
        out_specs=P(("sp", "tp"), None),
        check_vma=False,
    )
```
